32 devices in a mesh: sp: 16 (over z, y, x), dp: 2 (over core).
Axes of the slice: x: 2, y: 2, z: 4, core: 2. Of those that a mesh axis runs over, the one named last changes fastest.
Arguments:
- glu_value: bfloat16 [2, 8192, 512], P('dp', 'sp'), may hold values from -6 to 6
- glu_gate: bfloat16 [2, 8192, 512], P('dp', 'sp'), may hold values from -8 to 8
- cotangent: bfloat16 [2, 8192, 2048], P('dp', 'sp'), may hold values from -8 to 8
- conv_weight: float32 [31, 512], replicated, may hold values from -1 to 1
- norm_gain: float32 [512], replicated, may hold values from 0.1 to 1.9
- norm_shift: float32 [512], replicated, may hold values from -3 to 3
- out_weight: bfloat16 [2048, 512], P('dp'), may hold values from -0.25 to 0.25
Outputs:
- grad_value: bfloat16 [2, 8192, 512], P('dp', 'sp')
- grad_gate: bfloat16 [2, 8192, 512], P('dp', 'sp')
- grad_out_weight: float32 [2048, 512], P('dp')
- grad_conv: float32 [31, 512], replicated
- grad_gain: float32 [512], replicated
- grad_shift: float32 [512], replicated
The draws below stay inside these ranges and needn't reach their ends.
All inputs are finite; a program needn't handle non-finite values.
Results may differ from the reference program's by a relative error of at most 0.003.
Values may be sent and summed in bfloat16 or wider, within the bound.
No kernel may reach another device: no remote copies, remote signals or barrier semaphores. Data moves between devices by JAX's collectives and lax.ppermute only.
A program may use at most 64 MiB of HBM per device.

```python
import math
import jax
import jax.numpy as jnp
from jax import lax

D = 2048
C = 512
SPAN = 31
SEQS = 2
LENGTH = 8192
TOKENS = 16384


def strengthened(drawn, stream_key, source, target, shards_of, factor):
    owner, partner = [(jnp.arange(drawn.shape[dim]) // (drawn.shape[dim] // shards_of)).reshape([-1 if axis == dim else 1 for axis in range(drawn.ndim)]) for dim in (source, target)]
    chosen = jax.random.permutation(stream_key, shards_of)[partner]
    strong = (owner == chosen) | (owner == (partner + shards_of // 2) % shards_of)
    return jnp.where(strong, factor * drawn, drawn)


def steps_of(stream_key, extent, split, low, high):
    def one(position, shards_of):
        heights = jax.random.uniform(jax.random.fold_in(jax.random.fold_in(stream_key, 6), position), (shards_of,), jnp.float32, low / len(split), high / len(split))
        return jnp.repeat(jnp.exp(heights), extent[position] // shards_of).reshape((-1,) + (1,) * (len(extent) - position - 1))

    gain = one(*split[0])
    for cut in split[1:]:
        gain = gain * one(*cut)
    return gain


def scatter_about(stream_key, dims, width, limit, cuts=(), held_as=jnp.bfloat16):
    drawn = width * jax.random.normal(stream_key, dims, jnp.float32)
    if cuts:
        drawn = drawn * steps_of(stream_key, dims, cuts, -0.22, 0.18)
    return jnp.clip(drawn, -limit, limit).astype(held_as)


def bell_draw_with(own_key, dims, width, bound, split, heavy, kind=jnp.bfloat16):
    values = width * jax.random.normal(own_key, dims, jnp.float32)
    if split:
        values = values * steps_of(own_key, dims, split, -0.22, 0.18)
    return jnp.clip(strengthened(values, jax.random.fold_in(own_key, 3), *heavy), -bound, bound).astype(kind)


def setup_inputs(seed: int = 0) -> dict:
    keys = jax.random.split(jax.random.key(seed), 8)
    return {
        "glu_value": scatter_about(keys[0], (SEQS, LENGTH, C), 1.0, 6.0, ((0, 2), (1, 16))),
        "glu_gate": scatter_about(keys[1], (SEQS, LENGTH, C), 1.5, 8.0, ((0, 2), (1, 16))),
        "cotangent": bell_draw_with(keys[2], (SEQS, LENGTH, D), 1.0, 8.0, ((0, 2), (1, 16)), (1, 2, 16, 2.0)),
        "conv_weight": scatter_about(keys[3], (SPAN, C), SPAN ** -0.5, 1.0, (), jnp.float32),
        "norm_gain": jnp.clip(1.0 + 0.18 * jax.random.normal(keys[4], (C,), jnp.float32), 0.1, 1.9),
        "norm_shift": scatter_about(keys[5], (C,), 0.5, 3.0, (), jnp.float32),
        "out_weight": scatter_about(keys[6], (D, C), C ** -0.5, 0.25, ((0, 2),)),
    }


epsilon = 1e-06

def sequence_grads(value_rows, gate_rows, cotan_rows, conv_weight, norm_gain, norm_shift, out_weight):
    length = value_rows.shape[0]
    channels = value_rows.shape[1]
    tap_count = conv_weight.shape[0]
    value_full = value_rows.astype(jnp.float32)
    gate_full = gate_rows.astype(jnp.float32)
    sigmoid_gate = jax.nn.sigmoid(gate_full)
    gated = value_full * sigmoid_gate
    padded = jnp.concatenate([jnp.zeros((tap_count - 1, channels), jnp.float32), gated], axis=0)
    conv_rows = jnp.zeros((length, channels), jnp.float32)
    for offset in range(tap_count):
        conv_rows = conv_rows + conv_weight[offset] * padded[offset:offset + length]
    centred = conv_rows - lax.optimization_barrier(jnp.mean(conv_rows, axis=-1, keepdims=True))
    inv_std = lax.rsqrt(lax.optimization_barrier(jnp.mean(centred * centred, axis=-1, keepdims=True)) + epsilon)
    normed = centred * inv_std
    pre_act = normed * norm_gain + norm_shift
    sigmoid_pre = jax.nn.sigmoid(pre_act)
    act_rows = (pre_act * sigmoid_pre).astype(jnp.bfloat16)
    grad_act = jnp.dot(cotan_rows, out_weight, preferred_element_type=jnp.float32)
    grad_pre = grad_act * sigmoid_pre * (1.0 + pre_act * (1.0 - sigmoid_pre))
    grad_normed = grad_pre * norm_gain
    grad_conv_rows = inv_std * (grad_normed - lax.optimization_barrier(jnp.mean(grad_normed, axis=-1, keepdims=True)) - normed * lax.optimization_barrier(jnp.mean(grad_normed * normed, axis=-1, keepdims=True)))
    padded_grad = jnp.concatenate([grad_conv_rows, jnp.zeros((tap_count - 1, channels), jnp.float32)], axis=0)
    grad_gated = jnp.zeros((length, channels), jnp.float32)
    for offset in range(tap_count):
        start = tap_count - 1 - offset
        grad_gated = grad_gated + conv_weight[offset] * padded_grad[start:start + length]
    grad_taps = jnp.stack([lax.optimization_barrier(jnp.sum(grad_conv_rows * padded[offset:offset + length], axis=0)) for offset in range(tap_count)], axis=0)
    grad_value = (grad_gated * sigmoid_gate).astype(jnp.bfloat16)
    grad_gate = (grad_gated * value_full * sigmoid_gate * (1.0 - sigmoid_gate)).astype(jnp.bfloat16)
    grad_weight = jnp.dot(cotan_rows.T, act_rows, preferred_element_type=jnp.float32)
    return (grad_value, grad_gate, grad_weight, grad_taps, lax.optimization_barrier(jnp.sum(grad_pre * normed, axis=0)), lax.optimization_barrier(jnp.sum(grad_pre, axis=0)))

def reference(glu_value, glu_gate, cotangent, conv_weight, norm_gain, norm_shift, out_weight):

    def one_sequence(items):
        return sequence_grads(items[0], items[1], items[2], conv_weight, norm_gain, norm_shift, out_weight)
    results = lax.map(one_sequence, (glu_value, glu_gate, cotangent))
    scale = 1.0 / math.sqrt(TOKENS)
    grad_out_weight = lax.optimization_barrier(jnp.sum(results[2], axis=0)) * scale
    grad_conv = lax.optimization_barrier(jnp.sum(results[3], axis=0)) * scale
    grad_gain = lax.optimization_barrier(jnp.sum(results[4], axis=0)) * scale
    grad_shift = lax.optimization_barrier(jnp.sum(results[5], axis=0)) * scale
    return (results[0], results[1], grad_out_weight, grad_conv, grad_gain, grad_shift)
```

```python
import math

import jax
import jax.numpy as jnp
from jax import lax
from jax.sharding import PartitionSpec as P

epsilon = 1e-06


def from_behind(value, axis, by):
    count = lax.axis_size(axis)
    pairs = [(i, i + by) for i in range(count) if 0 <= i + by < count]
    return lax.ppermute(value, axis, pairs)


def exchange(value, axis, offset):
    count = lax.axis_size(axis)
    return lax.ppermute(value, axis, [(i, i ^ offset) for i in range(count)])


def levels_of(count):
    bits = count.bit_length() - 1
    return [(1 << low, 1 << min(2, bits - low)) for low in range(0, bits, 2)]


def digit(level):
    low, width = level
    return (lax.axis_index("sp") // low) % width


def reduce_level(total, level):
    low, width = level
    mine = digit(level)
    parts = total.reshape((width, total.shape[0] // width) + total.shape[1:])
    arrived = [
        exchange(
            lax.dynamic_index_in_dim(parts, mine ^ other, 0, False).astype(jnp.bfloat16),
            "sp",
            other * low,
        )
        for other in range(width - 1, 0, -1)
    ]
    kept = lax.dynamic_index_in_dim(parts, mine, 0, False)
    for part in arrived:
        kept = kept + part.astype(jnp.float32)
    return kept


def gather_level(rows, level):
    low, width = level
    mine = digit(level)
    pieces = [rows] + [None] * (width - 1)
    for other in range(width - 1, 0, -1):
        pieces[other] = exchange(rows, "sp", other * low)
    half = 1
    while half < width:
        swap = (mine // half) % 2 == 1
        paired = []
        for i in range(0, len(pieces), 2):
            first, second = pieces[i], pieces[i + 1]
            paired.append(
                jnp.where(
                    swap,
                    jnp.concatenate([second, first], axis=0),
                    jnp.concatenate([first, second], axis=0),
                )
            )
        pieces = paired
        half *= 2
    return pieces[0]


def tree(items):
    while len(items) > 1:
        items = [items[i] + items[i + 1] for i in range(0, len(items), 2)]
    return items[0]


def all_sum(value, axis, level):
    low, width = level
    return tree([value] + [exchange(value, axis, other * low) for other in range(1, width)])


def per_device(glu_value, glu_gate, cotangent, conv_weight, norm_gain, norm_shift, out_weight):
    value_rows = glu_value[0]
    gate_rows = glu_gate[0]
    cotan_rows = cotangent[0]
    length = value_rows.shape[0]
    channels = value_rows.shape[1]
    tap_count = conv_weight.shape[0]
    halo_rows = tap_count - 1
    count_sp = lax.axis_size("sp")
    count_dp = lax.axis_size("dp")
    scale = 1.0 / math.sqrt(length * count_sp * count_dp)
    prior_value, prior_gate = from_behind(
        (value_rows[length - halo_rows :], gate_rows[length - halo_rows :]), "sp", 1
    )
    value_ext = jnp.concatenate([prior_value, value_rows], axis=0).astype(jnp.float32)
    gate_ext = jnp.concatenate([prior_gate, gate_rows], axis=0).astype(jnp.float32)
    gated_ext = value_ext * jax.nn.sigmoid(gate_ext)
    conv_rows = jnp.zeros((length, channels), jnp.float32)
    for offset in range(tap_count):
        conv_rows = conv_rows + conv_weight[offset] * gated_ext[offset : offset + length]
    centred = conv_rows - jnp.mean(conv_rows, axis=-1, keepdims=True)
    inv_std = lax.rsqrt(jnp.mean(centred * centred, axis=-1, keepdims=True) + epsilon)
    normed = centred * inv_std
    pre_act = normed * norm_gain + norm_shift
    sigmoid_pre = jax.nn.sigmoid(pre_act)
    act_rows = (pre_act * sigmoid_pre).astype(jnp.bfloat16)
    columns = cotan_rows
    grad_act = jnp.dot(
        columns,
        lax.all_gather(out_weight, "dp", axis=0, tiled=True),
        preferred_element_type=jnp.float32,
    )
    grad_pre = grad_act * sigmoid_pre * (1.0 + pre_act * (1.0 - sigmoid_pre))
    grad_normed = grad_pre * norm_gain
    grad_conv_rows = inv_std * (
        grad_normed
        - jnp.mean(grad_normed, axis=-1, keepdims=True)
        - normed * jnp.mean(grad_normed * normed, axis=-1, keepdims=True)
    )
    later_grads = from_behind(grad_conv_rows[:halo_rows], "sp", -1)
    padded_grad = jnp.concatenate([grad_conv_rows, later_grads], axis=0)
    grad_gated = jnp.zeros((length, channels), jnp.float32)
    for offset in range(tap_count):
        start = tap_count - 1 - offset
        grad_gated = grad_gated + conv_weight[offset] * padded_grad[start : start + length]
    grad_taps = jnp.stack(
        [
            jnp.sum(grad_conv_rows * gated_ext[offset : offset + length], axis=0)
            for offset in range(tap_count)
        ],
        axis=0,
    )
    sigmoid_gate = jax.nn.sigmoid(gate_ext[halo_rows:])
    grad_value = (grad_gated * sigmoid_gate).astype(jnp.bfloat16)
    grad_gate = (grad_gated * value_ext[halo_rows:] * sigmoid_gate * (1.0 - sigmoid_gate)).astype(
        jnp.bfloat16
    )
    levels = levels_of(count_sp)
    product = lax.dot_general(
        cotan_rows, act_rows, (((0,), (0,)), ((), ())), preferred_element_type=jnp.float32
    )
    features = product.shape[0] // count_dp
    blocks = (product * scale).reshape(count_dp, features, channels)
    index_dp = lax.axis_index("dp")
    arrived = [
        exchange(lax.dynamic_index_in_dim(blocks, index_dp ^ other, 0, False), "dp", other)
        for other in range(1, count_dp)
    ]
    total = tree([lax.dynamic_index_in_dim(blocks, index_dp, 0, False)] + arrived)
    cut = 3 * features // 4
    if len(levels) > 1 and cut % (16 * count_sp) == 0 and (features - cut) % (16 * count_sp) == 0:
        colours = [(total[:cut], levels), (total[cut:], levels[1:] + levels[:1])]
    else:
        colours = [(total, levels)]
    states = [c[0] for c in colours]
    for step in range(len(levels)):
        states = [reduce_level(v, order[step]) for v, (_, order) in zip(states, colours)]
    states = [v.astype(jnp.bfloat16) for v in states]
    small = jnp.concatenate(
        [grad_taps, jnp.sum(grad_pre * normed, axis=0)[None], jnp.sum(grad_pre, axis=0)[None]]
    ) * scale
    small = all_sum(small, "dp", (1, count_dp))
    for step in reversed(range(len(levels))):
        states = [gather_level(v, order[step]) for v, (_, order) in zip(states, colours)]
        small = all_sum(small, "sp", levels[len(levels) - 1 - step])
    grad_out_weight = jnp.concatenate(states, axis=0).astype(jnp.float32)
    grad_conv, grad_gain, grad_shift = small[:tap_count], small[tap_count], small[tap_count + 1]
    return (grad_value[None], grad_gate[None], grad_out_weight, grad_conv, grad_gain, grad_shift)


def solution(mesh):
    in_specs = (
        P("dp", "sp", None),
        P("dp", "sp", None),
        P("dp", "sp", None),
        P(),
        P(),
        P(),
        P("dp", None),
    )
    out_specs = (P("dp", "sp", None), P("dp", "sp", None), P("dp", None), P(), P(), P())
    return jax.shard_map(
        per_device, mesh=mesh, in_specs=in_specs, out_specs=out_specs, check_vma=False
    )
```

```python
import functools
import math

import jax
import jax.numpy as jnp
from jax import lax
from jax.experimental import pallas as pl
from jax.experimental.pallas import tpu as pltpu
from jax.sharding import PartitionSpec as P

epsilon = 1e-06


def exchange(value, axis, offset):
    count = lax.axis_size(axis)
    return lax.ppermute(value, axis, [(i, i ^ offset) for i in range(count)])


def levels_of(count):
    bits = count.bit_length() - 1
    return [(1 << low, 1 << min(2, bits - low)) for low in range(0, bits, 2)]


def digit(level):
    low, width = level
    return (lax.axis_index("sp") // low) % width


def reduce_level(total, level):
    low, width = level
    mine = digit(level)
    parts = total.reshape((width, total.shape[0] // width) + total.shape[1:])
    arrived = [
        exchange(
            lax.dynamic_index_in_dim(parts, mine ^ other, 0, False).astype(jnp.bfloat16),
            "sp",
            other * low,
        )
        for other in range(width - 1, 0, -1)
    ]
    kept = lax.dynamic_index_in_dim(parts, mine, 0, False)
    for part in arrived:
        kept = kept + part.astype(jnp.float32)
    return kept


def gather_level(rows, level):
    low, width = level
    mine = digit(level)
    pieces = [rows] + [None] * (width - 1)
    for other in range(width - 1, 0, -1):
        pieces[other] = exchange(rows, "sp", other * low)
    half = 1
    while half < width:
        swap = (mine // half) % 2 == 1
        paired = []
        for i in range(0, len(pieces), 2):
            first, second = pieces[i], pieces[i + 1]
            paired.append(
                jnp.where(
                    swap,
                    jnp.concatenate([second, first], axis=0),
                    jnp.concatenate([first, second], axis=0),
                )
            )
        pieces = paired
        half *= 2
    return pieces[0]


def tree(items):
    while len(items) > 1:
        items = [items[i] + items[i + 1] for i in range(0, len(items), 2)]
    return items[0]


def all_sum(value, axis, level):
    low, width = level
    return tree([value] + [exchange(value, axis, other * low) for other in range(1, width)])


lanes = 128
sublanes = 8


def rounded_up(count, unit):
    return -(-count // unit) * unit


def fwd_kernel(value, gate, halo, cotan, weight, gain, shift, *rest, taps, pad, seg, eps, scale, others):
    sent = rest[: 1 if others else 0]
    own, gated, normed, inv_out, taps_in, conv, act, cot, arrive = rest[1 if others else 0 :]
    length, channels = value.shape
    groups = channels // lanes
    segments = length // seg
    rows = pad + seg
    copy = pltpu.make_async_copy(cotan, cot, arrive)
    copy.start()

    def gate_rows(v, g):
        return v.astype(jnp.float32) * jax.nn.sigmoid(g.astype(jnp.float32))

    for k in range(groups):
        cols = slice(k * lanes, (k + 1) * lanes)
        gated[k * rows : k * rows + pad, :] = gate_rows(halo[:pad, cols], halo[pad:, cols])
        for s in range(segments):
            at = (s * groups + k) * rows + pad
            block = gate_rows(value[s * seg : (s + 1) * seg, cols], gate[s * seg : (s + 1) * seg, cols])
            gated[at : at + seg, :] = block
            if s + 1 < segments:
                to = ((s + 1) * groups + k) * rows
                gated[to : to + pad, :] = block[seg - pad :]
            taps_in[(s * groups + k) * pad : (s * groups + k) * pad + taps, :] = weight[:, cols]
    tap = [taps_in[pl.ds(j, sublanes, stride=pad), :] for j in range(taps)]
    unit = 8

    def conv_block(i, carry):
        base = i * unit
        sums = [None] * unit
        for m in range(unit + taps - 1):
            row = gated[pl.ds(base + (pad - taps + 1) + m, sublanes, stride=rows), :]
            for u in range(unit):
                j = m - u
                if 0 <= j < taps:
                    term = tap[j] * row
                    sums[u] = term if sums[u] is None else sums[u] + term
        for u in range(unit):
            conv[pl.ds(base + u, sublanes, stride=seg), :] = sums[u]
        return carry

    lax.fori_loop(0, seg // unit, conv_block, 0)
    chunk = 32
    for s in range(segments):

        def norm_block(i, carry, s=s):
            base = pl.multiple_of(i * chunk, chunk)
            out = pl.multiple_of(s * seg + i * chunk, chunk)
            parts = [conv[pl.ds((s * groups + k) * seg + base, chunk), :] for k in range(groups)]
            mean = jnp.sum(sum(parts), axis=-1, keepdims=True) / channels
            parts = [p - mean for p in parts]
            var = jnp.sum(sum(p * p for p in parts), axis=-1, keepdims=True) / channels
            inv = lax.rsqrt(var + eps)
            inv_out[pl.ds(out, chunk), :] = jnp.broadcast_to(inv, (chunk, lanes))
            for k in range(groups):
                cols = slice(k * lanes, (k + 1) * lanes)
                n = parts[k] * inv
                normed[pl.ds(out, chunk), cols] = n
                pre = n * gain[:, cols] + shift[:, cols]
                act[pl.ds(out, chunk), cols] = (pre * jax.nn.sigmoid(pre)).astype(jnp.bfloat16)
            return carry

        lax.fori_loop(0, seg // chunk, norm_block, 0)
    copy.wait()
    features = own.shape[0]
    index = lax.axis_index("dp")
    step = min(features, 256)
    for other in list(range(1, others + 1)) + [0]:
        for f in range(0, features, step):
            at = pl.multiple_of((index ^ other) * features + f, lanes)
            part = lax.dot_general(
                cot[:, pl.ds(at, step)],
                act[...],
                (((0,), (0,)), ((), ())),
                preferred_element_type=jnp.float32,
            )
            if other:
                sent[0][other - 1, f : f + step, :] = part * scale
            else:
                own[f : f + step, :] = part * scale


def bwd_kernel(cotan, normed, inv_in, gain, shift, *rest, seg, scale, pieces):
    weights = rest[:pieces]
    grads, head, sums, act = rest[pieces:]
    length, channels = normed.shape
    groups = channels // lanes
    segments = length // seg
    features = weights[0].shape[0]
    index = lax.axis_index("dp")
    for other in range(pieces):
        at = pl.multiple_of((index ^ other) * features, lanes)
        part = jnp.dot(
            cotan[:, pl.ds(at, features)], weights[other][...], preferred_element_type=jnp.float32
        )
        act[...] = part if other == 0 else act[...] + part
    chunk = 32
    total = tuple(jnp.zeros((sublanes, lanes), jnp.float32) for _ in range(2 * groups))
    for s in range(segments):

        def grad_block(i, carry, s=s):
            base = pl.multiple_of(i * chunk, chunk)
            at = pl.multiple_of(s * seg + i * chunk, chunk)
            inv = inv_in[pl.ds(at, chunk), :]
            carry = list(carry)
            n, gn = [], []
            for k in range(groups):
                cols = slice(k * lanes, (k + 1) * lanes)
                nk = normed[pl.ds(at, chunk), cols]
                pre = nk * gain[:, cols] + shift[:, cols]
                sig = jax.nn.sigmoid(pre)
                grad_pre = act[pl.ds(at, chunk), cols] * sig * (1.0 + pre * (1.0 - sig))
                by_gain = (grad_pre * nk).reshape(chunk // sublanes, sublanes, lanes)
                by_shift = grad_pre.reshape(chunk // sublanes, sublanes, lanes)
                carry[k] = carry[k] + jnp.sum(by_gain, axis=0)
                carry[groups + k] = carry[groups + k] + jnp.sum(by_shift, axis=0)
                n.append(nk)
                gn.append(grad_pre * gain[:, cols])
            mean = jnp.sum(sum(gn), axis=-1, keepdims=True) / channels
            slope = jnp.sum(sum(a * b for a, b in zip(gn, n)), axis=-1, keepdims=True) / channels
            for k in range(groups):
                grads[pl.ds((s * groups + k) * seg + base, chunk), :] = inv * (
                    gn[k] - mean - n[k] * slope
                )
            return tuple(carry)

        total = lax.fori_loop(0, seg // chunk, grad_block, total)
    pad = head.shape[0]
    for k in range(groups):
        cols = slice(k * lanes, (k + 1) * lanes)
        head[:, cols] = grads[k * seg : k * seg + pad, :]
        for row in range(2):
            sums[row : row + 1, cols] = (
                jnp.sum(total[row * groups + k], axis=0, keepdims=True) * scale
            )


def taps_kernel(grads, gated, sums, small, spread, *, taps, pad, seg, scale):
    rows = pad + seg
    groups = small.shape[1] // lanes
    unit = 4

    def tap_block(i, carry):
        base = i * unit
        carry = list(carry)
        grad = [grads[pl.ds(base + u, sublanes, stride=seg), :] for u in range(unit)]
        for m in range(unit + taps - 1):
            row = gated[pl.ds(base + (pad - taps + 1) + m, sublanes, stride=rows), :]
            for u in range(unit):
                j = m - u
                if 0 <= j < taps:
                    carry[j] = carry[j] + grad[u] * row
        return tuple(carry)

    zero = jnp.zeros((sublanes, lanes), jnp.float32)
    total = lax.fori_loop(0, seg // unit, tap_block, (zero,) * taps)
    for j in range(taps):
        spread[pl.ds(j, sublanes, stride=pad), :] = total[j] * scale
    small[...] = jnp.zeros_like(small)
    for k in range(groups):
        cols = slice(k * lanes, (k + 1) * lanes)
        small[:taps, cols] = sum(
            spread[b * pad : b * pad + taps, :] for b in range(k, sublanes, groups)
        )
        small[taps : taps + 2, cols] = sums[:, cols]


def input_kernel(grads, halo, weight, value, gate, grad_value, grad_gate, taps_in, tail, conv, *, taps, pad, seg):
    length, channels = value.shape
    groups = channels // lanes
    segments = length // seg
    for k in range(groups):
        cols = slice(k * lanes, (k + 1) * lanes)
        for s in range(segments):
            b = s * groups + k
            taps_in[b * pad : b * pad + taps, :] = weight[:, cols]
            tail[b * 2 * pad : b * 2 * pad + pad, :] = grads[(b + 1) * seg - pad : (b + 1) * seg, :]
            if s + 1 < segments:
                after = grads[(b + groups) * seg : (b + groups) * seg + pad, :]
            else:
                after = halo[:, cols]
            tail[b * 2 * pad + pad : (b + 1) * 2 * pad, :] = after
    tap = [taps_in[pl.ds(j, sublanes, stride=pad), :] for j in range(taps)]
    unit = 8

    def block_of(source, stride, offset):
        def conv_block(i, carry):
            base = i * unit
            sums = [None] * unit
            for m in range(unit + taps - 1):
                row = source[pl.ds(base + m, sublanes, stride=stride), :]
                for u in range(unit):
                    j = taps - 1 - (m - u)
                    if 0 <= j < taps:
                        term = tap[j] * row
                        sums[u] = term if sums[u] is None else sums[u] + term
            for u in range(unit):
                conv[pl.ds(offset + base + u, sublanes, stride=seg), :] = sums[u]
            return carry

        return conv_block

    lax.fori_loop(0, (seg - pad) // unit, block_of(grads, seg, 0), 0)
    lax.fori_loop(0, pad // unit, block_of(tail, 2 * pad, seg - pad), 0)
    chunk = 32
    for s in range(segments):

        def out_block(i, carry, s=s):
            base = pl.multiple_of(i * chunk, chunk)
            at = pl.multiple_of(s * seg + i * chunk, chunk)
            for k in range(groups):
                cols = slice(k * lanes, (k + 1) * lanes)
                grad = conv[pl.ds((s * groups + k) * seg + base, chunk), :]
                sig = jax.nn.sigmoid(gate[pl.ds(at, chunk), cols].astype(jnp.float32))
                by_value = grad * sig
                grad_value[pl.ds(at, chunk), cols] = by_value.astype(jnp.bfloat16)
                grad_gate[pl.ds(at, chunk), cols] = (
                    by_value * value[pl.ds(at, chunk), cols].astype(jnp.float32) * (1.0 - sig)
                ).astype(jnp.bfloat16)
            return carry

        lax.fori_loop(0, seg // chunk, out_block, 0)


def in_vmem(count):
    return [pl.BlockSpec(memory_space=pltpu.VMEM)] * count


def f32(*shape):
    return jax.ShapeDtypeStruct(shape, jnp.float32)


def per_device(glu_value, glu_gate, cotangent, conv_weight, norm_gain, norm_shift, out_weight):
    value_rows = glu_value[0]
    gate_rows = glu_gate[0]
    cotan_rows = cotangent[0]
    length, channels = value_rows.shape
    taps = conv_weight.shape[0]
    features = out_weight.shape[0]
    count_sp = lax.axis_size("sp")
    count_dp = lax.axis_size("dp")
    scale = 1.0 / math.sqrt(length * count_sp * count_dp)
    pad = rounded_up(taps, 16)
    seg = length * (channels // lanes) // sublanes
    gain = norm_gain[None]
    shift = norm_shift[None]
    blocks = length // seg * (channels // lanes)

    weights = [out_weight] + [exchange(out_weight, "dp", k) for k in range(1, count_dp)]
    halo = lax.ppermute(
        jnp.concatenate([value_rows[length - pad :], gate_rows[length - pad :]], axis=0),
        "sp",
        [(i, i + 1) for i in range(count_sp - 1)],
    )
    others = count_dp - 1
    sent_shape = [f32(others, features, channels)] if others else []
    outs = pl.pallas_call(
        functools.partial(
            fwd_kernel, taps=taps, pad=pad, seg=seg, eps=epsilon, scale=scale, others=others
        ),
        out_shape=sent_shape
        + [
            f32(features, channels),
            f32(blocks * (pad + seg), lanes),
            f32(length, channels),
            f32(length, lanes),
        ],
        in_specs=in_vmem(3) + [pl.BlockSpec(memory_space=pl.ANY)] + in_vmem(3),
        out_specs=in_vmem(len(sent_shape) + 4),
        scratch_shapes=[
            pltpu.VMEM((blocks * pad, lanes), jnp.float32),
            pltpu.VMEM((blocks * seg, lanes), jnp.float32),
            pltpu.VMEM((length, channels), jnp.bfloat16),
            pltpu.VMEM(cotan_rows.shape, jnp.bfloat16),
            pltpu.SemaphoreType.DMA,
        ],
        name="forward",
    )(value_rows, gate_rows, halo, cotan_rows, conv_weight, gain, shift)
    own, gated, normed, inv = outs[-4:]
    arrived = [exchange(outs[0][k - 1], "dp", k) for k in range(1, count_dp)]

    grads, head, sums = pl.pallas_call(
        functools.partial(bwd_kernel, seg=seg, scale=scale, pieces=count_dp),
        out_shape=[f32(blocks * seg, lanes), f32(pad, channels), f32(2, channels)],
        in_specs=in_vmem(5 + count_dp),
        out_specs=in_vmem(3),
        scratch_shapes=[pltpu.VMEM((length, channels), jnp.float32)],
        name="backward",
    )(cotan_rows, normed, inv, gain, shift, *weights)
    later = lax.ppermute(head, "sp", [(i, i - 1) for i in range(1, count_sp)])
    small = pl.pallas_call(
        functools.partial(taps_kernel, taps=taps, pad=pad, seg=seg, scale=scale),
        out_shape=f32(rounded_up(taps + 2, 8), channels),
        in_specs=in_vmem(3),
        out_specs=in_vmem(1)[0],
        scratch_shapes=[pltpu.VMEM((blocks * pad, lanes), jnp.float32)],
        name="taps",
    )(grads, gated, sums)
    grad_value, grad_gate = pl.pallas_call(
        functools.partial(input_kernel, taps=taps, pad=pad, seg=seg),
        out_shape=[jax.ShapeDtypeStruct((length, channels), jnp.bfloat16)] * 2,
        in_specs=in_vmem(5),
        out_specs=in_vmem(2),
        scratch_shapes=[
            pltpu.VMEM((blocks * pad, lanes), jnp.float32),
            pltpu.VMEM((blocks * 2 * pad, lanes), jnp.float32),
            pltpu.VMEM((blocks * seg, lanes), jnp.float32),
        ],
        name="inputs",
    )(grads, later, conv_weight, value_rows, gate_rows)

    levels = levels_of(count_sp)
    total = tree([own] + arrived)
    cut = 3 * features // 4
    if len(levels) > 1 and cut % (16 * count_sp) == 0 and (features - cut) % (16 * count_sp) == 0:
        colours = [(total[:cut], levels), (total[cut:], levels[1:] + levels[:1])]
    else:
        colours = [(total, levels)]
    states = [c[0] for c in colours]
    for step in range(len(levels)):
        states = [reduce_level(v, order[step]) for v, (_, order) in zip(states, colours)]
    states = [v.astype(jnp.bfloat16) for v in states]
    small = all_sum(small, "dp", (1, count_dp))
    for step in reversed(range(len(levels))):
        states = [gather_level(v, order[step]) for v, (_, order) in zip(states, colours)]
        small = all_sum(small, "sp", levels[len(levels) - 1 - step])
    grad_out_weight = jnp.concatenate(states, axis=0).astype(jnp.float32)
    return (
        grad_value[None],
        grad_gate[None],
        grad_out_weight,
        small[:taps],
        small[taps],
        small[taps + 1],
    )


def solution(mesh):
    in_specs = (
        P("dp", "sp", None),
        P("dp", "sp", None),
        P("dp", "sp", None),
        P(),
        P(),
        P(),
        P("dp", None),
    )
    out_specs = (P("dp", "sp", None), P("dp", "sp", None), P("dp", None), P(), P(), P())
    return jax.shard_map(
        per_device, mesh=mesh, in_specs=in_specs, out_specs=out_specs, check_vma=False
    )
```

```python
import functools
import math

import jax
import jax.numpy as jnp
from jax import lax
from jax.experimental import pallas as pl
from jax.experimental.pallas import tpu as pltpu
from jax.sharding import PartitionSpec as P

epsilon = 1e-06


def exchange(value, offset_of):
    count_sp = lax.axis_size("sp")
    count_dp = lax.axis_size("dp")
    pairs = []
    for d in range(count_dp):
        over_sp, over_dp = offset_of(d)
        for s in range(count_sp):
            pairs.append((s * count_dp + d, (s ^ over_sp) * count_dp + (d ^ over_dp)))
    return lax.ppermute(value, ("sp", "dp"), pairs)


def levels_of(count_sp, turn):
    bits = count_sp.bit_length() - 1
    levels = [(1 << low, 1 << min(2, bits - low)) for low in range(0, bits, 2)]
    if len({width for _, width in levels}) > 1:
        return levels
    turn %= max(len(levels), 1)
    return levels[turn:] + levels[:turn]


def digit(step):
    low = jnp.int32(1)
    for d in range(lax.axis_size("dp")):
        mine = levels_of(lax.axis_size("sp"), d)[step][0]
        low = jnp.where(lax.axis_index("dp") == d, mine, low)
    return (lax.axis_index("sp") // low) % width_of(step)


def width_of(step):
    return levels_of(lax.axis_size("sp"), 0)[step][1]


def exchange_digit(value, step, other):
    count_sp = lax.axis_size("sp")
    return exchange(value, lambda d: (levels_of(count_sp, d)[step][0] * other, 0))


def row_block(value, index, count):
    rows = value.shape[0] // count
    return lax.dynamic_slice_in_dim(value, index * rows, rows, 0)


def reduce_level(total, step, kind):
    width = width_of(step)
    mine = digit(step)
    arrived = [
        exchange_digit(row_block(total, mine ^ other, width).astype(kind), step, other)
        for other in range(width - 1, 0, -1)
    ]
    kept = row_block(total, mine, width)
    for part in arrived:
        kept = kept + part.astype(jnp.float32)
    return kept


def tree(items):
    while len(items) > 1:
        items = [items[i] + items[i + 1] for i in range(0, len(items), 2)]
    return items[0]


def two_halves(value):
    first = value.astype(jnp.bfloat16)
    return jnp.concatenate([first, (value - first.astype(jnp.float32)).astype(jnp.bfloat16)], axis=0)


def gather_level(rows, small, step):
    width = width_of(step)
    mine = digit(step)
    count = rows.shape[0]
    both = jnp.concatenate([rows, two_halves(small)], axis=0)
    pieces = [both] + [None] * (width - 1)
    for other in range(width - 1, 0, -1):
        pieces[other] = exchange_digit(both, step, other)
    half = small.shape[0]
    small = tree(
        [
            p[count : count + half].astype(jnp.float32) + p[count + half :].astype(jnp.float32)
            for p in pieces
        ]
    )
    pieces = [p[:count] for p in pieces]
    bit = 1
    while bit < width:
        swap = (mine // bit) % 2 == 1
        pieces = [
            jnp.where(
                swap,
                jnp.concatenate([pieces[i + 1], pieces[i]], axis=0),
                jnp.concatenate([pieces[i], pieces[i + 1]], axis=0),
            )
            for i in range(0, len(pieces), 2)
        ]
        bit *= 2
    return pieces[0], small


lanes = 128
sublanes = 8


def rounded_up(count, unit):
    return -(-count // unit) * unit


def strided(first, count):
    return pl.ds(first, count, stride=sublanes)


def tile(row):
    return pl.ds(pl.multiple_of(row * sublanes, sublanes), sublanes)


def grad_weight(out, cotan, act, block, scale):
    features = out.shape[0]
    step = min(features, 256)
    for f in range(0, features, step):
        at = pl.multiple_of(block * features + f, lanes)
        part = lax.dot_general(
            cotan[:, pl.ds(at, step)],
            act[...],
            (((0,), (0,)), ((), ())),
            preferred_element_type=jnp.float32,
        )
        out[f : f + step, :] = (part * scale).astype(out.dtype)


def fwd_kernel(value, gate, halo, cotan, weight, gain, shift, *rest, taps, pad, seg, eps, scale, others):
    sent = rest[:others]
    act, gated, normed, inv_out, taps_in, conv = rest[others:]
    length, channels = value.shape
    groups = channels // lanes
    segments = length // seg

    def gate_rows(v, g):
        return v.astype(jnp.float32) * jax.nn.sigmoid(g.astype(jnp.float32))

    for k in range(groups):
        cols = slice(k * lanes, (k + 1) * lanes)
        gated[strided(k, pad), :] = gate_rows(halo[:pad, cols], halo[pad:, cols])
        for s in range(segments):
            b = s * groups + k
            block = gate_rows(value[s * seg : (s + 1) * seg, cols], gate[s * seg : (s + 1) * seg, cols])
            gated[strided(pad * sublanes + b, seg), :] = block
            if s + 1 < segments:
                gated[strided(b + groups, pad), :] = block[seg - pad :]
            taps_in[strided(b, taps), :] = weight[:, cols]
    tap = [taps_in[tile(j), :] for j in range(taps)]
    unit = 16

    def conv_block(i, carry):
        base = i * unit
        sums = [None] * unit
        for m in range(unit + taps - 1):
            row = gated[tile(base + (pad - taps + 1) + m), :]
            for u in range(unit):
                j = m - u
                if 0 <= j < taps:
                    term = tap[j] * row
                    sums[u] = term if sums[u] is None else sums[u] + term
        for u in range(unit):
            conv[tile(base + u), :] = sums[u]
        return carry

    lax.fori_loop(0, seg // unit, conv_block, 0)
    chunk = 128
    for s in range(segments):

        def norm_block(i, carry, s=s):
            base = pl.multiple_of(i * chunk, chunk)
            out = pl.multiple_of(s * seg + i * chunk, chunk)
            parts = [
                conv[strided(base * sublanes + s * groups + k, chunk), :] for k in range(groups)
            ]
            mean = jnp.sum(sum(parts), axis=-1, keepdims=True) / channels
            parts = [p - mean for p in parts]
            var = jnp.sum(sum(p * p for p in parts), axis=-1, keepdims=True) / channels
            inv = lax.rsqrt(var + eps)
            inv_out[pl.ds(out, chunk), :] = jnp.broadcast_to(inv, (chunk, lanes))
            for k in range(groups):
                cols = slice(k * lanes, (k + 1) * lanes)
                n = parts[k] * inv
                normed[pl.ds(out, chunk), cols] = n
                pre = n * gain[:, cols] + shift[:, cols]
                act[pl.ds(out, chunk), cols] = (pre * jax.nn.sigmoid(pre)).astype(jnp.bfloat16)
            return carry

        lax.fori_loop(0, seg // chunk, norm_block, 0)
    for other in range(1, others + 1):
        grad_weight(sent[other - 1], cotan, act, lax.axis_index("dp") ^ other, scale)


def bwd_kernel(cotan, act, normed, inv_in, gain, shift, *rest, seg, scale, pieces):
    weights = rest[:pieces]
    own, grads, head, sums, grad_act = rest[pieces:]
    length, channels = normed.shape
    groups = channels // lanes
    segments = length // seg
    features = weights[0].shape[0]
    index = lax.axis_index("dp")
    grad_weight(own, cotan, act, index, scale)
    for other in range(pieces):
        at = pl.multiple_of((index ^ other) * features, lanes)
        part = jnp.dot(
            cotan[:, pl.ds(at, features)], weights[other][...], preferred_element_type=jnp.float32
        )
        grad_act[...] = part if other == 0 else grad_act[...] + part
    chunk = 128
    total = tuple(jnp.zeros((sublanes, lanes), jnp.float32) for _ in range(2 * groups))
    for s in range(segments):

        def grad_block(i, carry, s=s):
            base = pl.multiple_of(i * chunk, chunk)
            at = pl.multiple_of(s * seg + i * chunk, chunk)
            inv = inv_in[pl.ds(at, chunk), :]
            carry = list(carry)
            n, gn = [], []
            for k in range(groups):
                cols = slice(k * lanes, (k + 1) * lanes)
                nk = normed[pl.ds(at, chunk), cols]
                pre = nk * gain[:, cols] + shift[:, cols]
                sig = jax.nn.sigmoid(pre)
                grad_pre = grad_act[pl.ds(at, chunk), cols] * sig * (1.0 + pre * (1.0 - sig))
                by_gain = (grad_pre * nk).reshape(chunk // sublanes, sublanes, lanes)
                by_shift = grad_pre.reshape(chunk // sublanes, sublanes, lanes)
                carry[k] = carry[k] + jnp.sum(by_gain, axis=0)
                carry[groups + k] = carry[groups + k] + jnp.sum(by_shift, axis=0)
                n.append(nk)
                gn.append(grad_pre * gain[:, cols])
            mean = jnp.sum(sum(gn), axis=-1, keepdims=True) / channels
            slope = jnp.sum(sum(a * b for a, b in zip(gn, n)), axis=-1, keepdims=True) / channels
            for k in range(groups):
                grads[strided(base * sublanes + s * groups + k, chunk), :] = inv * (
                    gn[k] - mean - n[k] * slope
                )
            return tuple(carry)

        total = lax.fori_loop(0, seg // chunk, grad_block, total)
    pad = head.shape[0]
    for k in range(groups):
        cols = slice(k * lanes, (k + 1) * lanes)
        head[:, cols] = grads[strided(k, pad), :]
        for row in range(2):
            sums[row : row + 1, cols] = (
                jnp.sum(total[row * groups + k], axis=0, keepdims=True) * scale
            )


def taps_kernel(grads, gated, sums, small, spread, *, taps, pad, seg, scale):
    groups = small.shape[1] // lanes
    unit = 4

    def tap_block(i, carry):
        base = i * unit
        carry = list(carry)
        grad = [grads[tile(base + u), :] for u in range(unit)]
        for m in range(unit + taps - 1):
            row = gated[tile(base + (pad - taps + 1) + m), :]
            for u in range(unit):
                j = m - u
                if 0 <= j < taps:
                    carry[j] = carry[j] + grad[u] * row
        return tuple(carry)

    zero = jnp.zeros((sublanes, lanes), jnp.float32)
    total = lax.fori_loop(0, seg // unit, tap_block, (zero,) * taps)
    for j in range(taps):
        spread[tile(j), :] = total[j] * scale
    small[...] = jnp.zeros_like(small)
    for k in range(groups):
        cols = slice(k * lanes, (k + 1) * lanes)
        small[:taps, cols] = sum(
            spread[strided(b, taps), :] for b in range(k, sublanes, groups)
        )
        small[taps : taps + 2, cols] = sums[:, cols]


def input_kernel(grads, halo, weight, value, gate, grad_value, grad_gate, taps_in, tail, conv, *, taps, pad, seg):
    length, channels = value.shape
    groups = channels // lanes
    segments = length // seg
    for k in range(groups):
        cols = slice(k * lanes, (k + 1) * lanes)
        for s in range(segments):
            b = s * groups + k
            taps_in[strided(b, taps), :] = weight[:, cols]
            after = grads[strided(b + groups, pad), :] if s + 1 < segments else halo[:, cols]
            tail[strided(pad * sublanes + b, pad), :] = after
    tail[: pad * sublanes, :] = grads[(seg - pad) * sublanes :, :]
    tap = [taps_in[tile(j), :] for j in range(taps)]
    unit = 16

    def block_of(source, offset):
        def conv_block(i, carry):
            base = i * unit
            sums = [None] * unit
            for m in range(unit + taps - 1):
                row = source[tile(base + m), :]
                for u in range(unit):
                    j = taps - 1 - (m - u)
                    if 0 <= j < taps:
                        term = tap[j] * row
                        sums[u] = term if sums[u] is None else sums[u] + term
            for u in range(unit):
                conv[tile(offset + base + u), :] = sums[u]
            return carry

        return conv_block

    lax.fori_loop(0, (seg - pad) // unit, block_of(grads, 0), 0)
    lax.fori_loop(0, pad // unit, block_of(tail, seg - pad), 0)
    chunk = 128
    for s in range(segments):

        def out_block(i, carry, s=s):
            base = pl.multiple_of(i * chunk, chunk)
            at = pl.multiple_of(s * seg + i * chunk, chunk)
            for k in range(groups):
                cols = slice(k * lanes, (k + 1) * lanes)
                grad = conv[strided(base * sublanes + s * groups + k, chunk), :]
                sig = jax.nn.sigmoid(gate[pl.ds(at, chunk), cols].astype(jnp.float32))
                by_value = grad * sig
                grad_value[pl.ds(at, chunk), cols] = by_value.astype(jnp.bfloat16)
                grad_gate[pl.ds(at, chunk), cols] = (
                    by_value * value[pl.ds(at, chunk), cols].astype(jnp.float32) * (1.0 - sig)
                ).astype(jnp.bfloat16)
            return carry

        lax.fori_loop(0, seg // chunk, out_block, 0)


def in_vmem(count):
    return [pl.BlockSpec(memory_space=pltpu.VMEM)] * count


def f32(*shape):
    return jax.ShapeDtypeStruct(shape, jnp.float32)


def small_part(small, count_dp):
    if count_dp == 1:
        return small
    half = small.shape[0] // 2
    index = lax.axis_index("dp") % 2
    other = exchange(lax.dynamic_slice_in_dim(small, (1 - index) * half, half, 0), lambda d: (0, 1))
    return lax.dynamic_slice_in_dim(small, index * half, half, 0) + other


def small_whole(mine, count_dp):
    for bit in bits_of(count_dp)[1:]:
        mine = mine + exchange(mine, lambda d, bit=bit: (0, bit))
    if count_dp == 1:
        return mine
    other = exchange(mine, lambda d: (0, 1))
    first = lax.axis_index("dp") % 2 == 0
    return jnp.where(
        first, jnp.concatenate([mine, other], axis=0), jnp.concatenate([other, mine], axis=0)
    )


def bits_of(count):
    return [1 << b for b in range(count.bit_length() - 1)]


def per_device(glu_value, glu_gate, cotangent, conv_weight, norm_gain, norm_shift, out_weight):
    value_rows = glu_value[0]
    gate_rows = glu_gate[0]
    cotan_rows = cotangent[0]
    length, channels = value_rows.shape
    taps = conv_weight.shape[0]
    features = out_weight.shape[0]
    count_sp = lax.axis_size("sp")
    count_dp = lax.axis_size("dp")
    scale = 1.0 / math.sqrt(length * count_sp * count_dp)
    pad = rounded_up(taps, 16)
    seg = length * (channels // lanes) // sublanes
    gain = norm_gain[None]
    shift = norm_shift[None]
    blocks = length // seg * (channels // lanes)

    weights = [out_weight] + [
        exchange(out_weight, lambda d, k=k: (0, k)) for k in range(1, count_dp)
    ]
    halo = lax.ppermute(
        jnp.concatenate([value_rows[length - pad :], gate_rows[length - pad :]], axis=0),
        "sp",
        [(i, i + 1) for i in range(count_sp - 1)],
    )
    others = count_dp - 1
    *sent, act, gated, normed, inv = pl.pallas_call(
        functools.partial(
            fwd_kernel, taps=taps, pad=pad, seg=seg, eps=epsilon, scale=scale, others=others
        ),
        out_shape=[f32(features, channels)] * others
        + [
            jax.ShapeDtypeStruct((length, channels), jnp.bfloat16),
            f32((pad + seg) * sublanes, lanes),
            f32(length, channels),
            f32(length, lanes),
        ],
        in_specs=in_vmem(7),
        out_specs=in_vmem(others + 4),
        scratch_shapes=[
            pltpu.VMEM((pad * sublanes, lanes), jnp.float32),
            pltpu.VMEM((seg * sublanes, lanes), jnp.float32),
        ],
        name="forward",
    )(value_rows, gate_rows, halo, cotan_rows, conv_weight, gain, shift)
    arrived = [exchange(sent[k - 1], lambda d, k=k: (0, k)) for k in range(1, count_dp)]

    own, grads, head, sums = pl.pallas_call(
        functools.partial(bwd_kernel, seg=seg, scale=scale, pieces=count_dp),
        out_shape=[
            f32(features, channels),
            f32(seg * sublanes, lanes),
            f32(pad, channels),
            f32(2, channels),
        ],
        in_specs=in_vmem(6 + count_dp),
        out_specs=in_vmem(4),
        scratch_shapes=[pltpu.VMEM((length, channels), jnp.float32)],
        name="backward",
    )(cotan_rows, act, normed, inv, gain, shift, *weights)
    later = lax.ppermute(head, "sp", [(i, i - 1) for i in range(1, count_sp)])
    small = pl.pallas_call(
        functools.partial(taps_kernel, taps=taps, pad=pad, seg=seg, scale=scale),
        out_shape=f32(rounded_up(taps + 2, 8), channels),
        in_specs=in_vmem(3),
        out_specs=in_vmem(1)[0],
        scratch_shapes=[pltpu.VMEM((pad * sublanes, lanes), jnp.float32)],
        name="taps",
    )(grads, gated, sums)
    grad_value, grad_gate = pl.pallas_call(
        functools.partial(input_kernel, taps=taps, pad=pad, seg=seg),
        out_shape=[jax.ShapeDtypeStruct((length, channels), jnp.bfloat16)] * 2,
        in_specs=in_vmem(5),
        out_specs=in_vmem(2),
        scratch_shapes=[
            pltpu.VMEM((pad * sublanes, lanes), jnp.float32),
            pltpu.VMEM((2 * pad * sublanes, lanes), jnp.float32),
            pltpu.VMEM((seg * sublanes, lanes), jnp.float32),
        ],
        name="inputs",
    )(grads, later, conv_weight, value_rows, gate_rows)

    steps = len(levels_of(count_sp, 0))
    rows = tree([own] + arrived)
    for step in range(steps):
        rows = reduce_level(rows, step, jnp.bfloat16 if step == 0 else jnp.float32)
    rows = rows.astype(jnp.bfloat16)
    mine = small_part(small, count_dp)
    for step in reversed(range(steps)):
        rows, mine = gather_level(rows, mine, step)
    grad_out_weight = rows.astype(jnp.float32)
    small = small_whole(mine, count_dp)
    return (
        grad_value[None],
        grad_gate[None],
        grad_out_weight,
        small[:taps],
        small[taps],
        small[taps + 1],
    )


def solution(mesh):
    in_specs = (
        P("dp", "sp", None),
        P("dp", "sp", None),
        P("dp", "sp", None),
        P(),
        P(),
        P(),
        P("dp", None),
    )
    out_specs = (P("dp", "sp", None), P("dp", "sp", None), P("dp", None), P(), P(), P())
    return jax.shard_map(
        per_device, mesh=mesh, in_specs=in_specs, out_specs=out_specs, check_vma=False
    )
```
